32 devices in a mesh: dp: 4 (over y, x), kv: 4 (over z), tp: 2 (over core).
Axes of the slice: x: 2, y: 2, z: 4, core: 2. Of those that a mesh axis runs over, the one named last changes fastest.
Arguments:
- layer_input: bfloat16 [128, 4096], P('dp', ('kv', 'tp')), parts along dimension 0, may hold values from -22 to 22
- gate_weight: bfloat16 [4096, 2048], P(('kv', 'tp')), may hold values from -0.09375 to 0.09375
- value_weight: bfloat16 [4096, 2048], P(('kv', 'tp')), may hold values from -0.09375 to 0.09375
- write_weight: bfloat16 [4096, 256], P(('kv', 'tp')), may hold values from -0.09375 to 0.09375
- read_weight: bfloat16 [4096, 256], P(('kv', 'tp')), may hold values from -0.09375 to 0.09375
- step_weight: bfloat16 [4096, 32], P(('kv', 'tp')), may hold values from -0.09375 to 0.09375
- value_taps: bfloat16 [4, 2048], replicated, may hold values from -3 to 3
- write_taps: bfloat16 [4, 256], replicated, may hold values from -3 to 3
- read_taps: bfloat16 [4, 256], replicated, may hold values from -3 to 3
- past_values: bfloat16 [128, 3, 2048], P(('dp', 'kv', 'tp')), parts along dimension 0, may hold values from -6 to 6
- past_writes: bfloat16 [128, 3, 256], P(('dp', 'kv', 'tp')), parts along dimension 0, may hold values from -6 to 6
- past_reads: bfloat16 [128, 3, 256], P(('dp', 'kv', 'tp')), parts along dimension 0, may hold values from -6 to 6
- step_bias: float32 [32], replicated, may hold values from -4 to -1
- decay_log: float32 [32], replicated, may hold values from 0 to 2.77
- skip_scale: float32 [32], replicated, may hold values from 0.5 to 2
- state_past: float32 [128, 32, 64, 128], P(('dp', 'kv', 'tp')), parts along dimension 0, may hold values from -3 to 3
- mixer_gain: float32 [2048], replicated, may hold values from 0.1 to 1.9
- out_weight: bfloat16 [2048, 4096], P(None, ('kv', 'tp')), may hold values from -0.125 to 0.125
- norm1_gain: float32 [4096], replicated, may hold values from 0.24 to 3.7
- up_weight: bfloat16 [4096, 16384], P(None, ('kv', 'tp')), may hold values from -0.09375 to 0.09375
- down_weight: bfloat16 [16384, 4096], P(('kv', 'tp')), may hold values from -0.0625 to 0.0625
- norm2_gain: float32 [4096], replicated, may hold values from 0.1 to 1.9
Outputs:
- layer_output: bfloat16 [128, 4096], P('dp', ('kv', 'tp')), parts along dimension 0
- state_next: float32 [128, 32, 64, 128], P(('dp', 'kv', 'tp')), parts along dimension 0
The draws below stay inside these ranges and needn't reach their ends.
There are 4 independent parts, one for each index of `dp`. The reference program is written for one: setup_inputs(seed, part) draws one part's arguments, and reference() takes and returns one part's arrays. A program takes and returns all parts, laid end to end along the dimension named above; an argument that names none is the same for every part. Nothing has to cross between parts.
All inputs are finite; a program needn't handle non-finite values.
Results may differ from the reference program's by a relative error of at most 0.012.
Values may be sent and summed in bfloat16 or wider, within the bound.
A program may use at most 128 MiB of HBM per device.

```python
import math
import jax
import jax.numpy as jnp
from jax import lax

D = 4096
HEADS = 32
HEAD_DIM = 64
STATE_DIM = 128
GROUPS = 2
CONV_TAPS = 4
FF = 16384
INNER = 2048
SEQS = 32


def draw_layer_input(key, part):
    first_key, second_key = jax.random.split(jax.random.fold_in(key, 11), 2)
    ramp = jnp.exp(jnp.linspace(math.log(0.4), math.log(2.5), D)).astype(jnp.float32)
    rough = jnp.exp(jax.random.uniform(second_key, (D,), jnp.float32, -0.35, 0.35))
    base = jnp.clip(jax.random.normal(first_key, (SEQS, D), jnp.float32), -6.0, 6.0)
    return (base * ramp[None, :] * rough[None, :]).astype(jnp.bfloat16)


def draw_norm1_gain(key, part):
    first_key = jax.random.fold_in(key, 23)
    ramp = jnp.exp(jnp.linspace(math.log(0.4), math.log(2.5), D)).astype(jnp.float32)
    rough = jnp.exp(jax.random.uniform(first_key, (D,), jnp.float32, -0.2, 0.2))
    return (ramp * rough).astype(jnp.float32)


def with_spikes(entries, own_key, source, target, parts, factor):
    def block_of(dim):
        return (jnp.arange(entries.shape[dim]) // (entries.shape[dim] // parts)).reshape((-1,) + (1,) * (entries.ndim - 1 - dim))

    near = jax.random.permutation(own_key, parts)[block_of(target)]
    other_side = (block_of(target) + parts // 2) % parts
    return jnp.where((block_of(source) == near) | (block_of(source) == other_side), factor * entries, entries)


def steps_of(rng, shape, cuts, smallest, high):
    def one(dim, shards_of):
        steps = jax.random.uniform(jax.random.fold_in(jax.random.fold_in(rng, 6), dim), (shards_of,), jnp.float32, smallest / len(cuts), high / len(cuts))
        return jnp.repeat(jnp.exp(steps), shape[dim] // shards_of).reshape((-1,) + (1,) * (len(shape) - dim - 1))

    level = one(*cuts[0])
    for cut in cuts[1:]:
        level = level * one(*cut)
    return level


def normal_values(rng, extent, spread, most, cuts=(), kind=jnp.bfloat16):
    values = spread * jax.random.normal(rng, extent, jnp.float32)
    if cuts:
        values = values * steps_of(rng, extent, cuts, -0.22, 0.18)
    return jnp.clip(values, -most, most).astype(kind)


def gaussian_with(stream_key, dims, width, bound, shards, heavy, kind=jnp.bfloat16):
    values = width * jax.random.normal(stream_key, dims, jnp.float32)
    if shards:
        values = values * steps_of(stream_key, dims, shards, -0.22, 0.18)
    return jnp.clip(with_spikes(values, jax.random.fold_in(stream_key, 3), *heavy), -bound, bound).astype(kind)


def setup_inputs(seed: int = 0, part: int = 0) -> dict:
    key_of = jax.random.split(jax.random.key(seed), 23)
    own_keys = jax.random.split(jax.random.fold_in(key_of[22], part), 23)
    return {
        "layer_input": draw_layer_input(jax.random.fold_in(jax.random.fold_in(key_of[22], part), 71), part),
        "gate_weight": normal_values(key_of[1], (D, INNER), D ** -0.5, 0.09375, ((0, 8),)),
        "value_weight": normal_values(key_of[2], (D, INNER), D ** -0.5, 0.09375, ((0, 8),)),
        "write_weight": normal_values(key_of[3], (D, GROUPS * STATE_DIM), D ** -0.5, 0.09375, ((0, 8),)),
        "read_weight": normal_values(key_of[4], (D, GROUPS * STATE_DIM), D ** -0.5, 0.09375, ((0, 8),)),
        "step_weight": normal_values(key_of[5], (D, HEADS), D ** -0.5, 0.09375, ((0, 8),)),
        "value_taps": normal_values(key_of[6], (CONV_TAPS, INNER), CONV_TAPS ** -0.5, 3.0),
        "write_taps": normal_values(key_of[7], (CONV_TAPS, GROUPS * STATE_DIM), CONV_TAPS ** -0.5, 3.0),
        "read_taps": normal_values(key_of[8], (CONV_TAPS, GROUPS * STATE_DIM), CONV_TAPS ** -0.5, 3.0),
        "past_values": normal_values(own_keys[9], (SEQS, CONV_TAPS - 1, INNER), 1.0, 6.0, ((0, 8),)),
        "past_writes": normal_values(own_keys[10], (SEQS, CONV_TAPS - 1, GROUPS * STATE_DIM), 1.0, 6.0, ((0, 8),)),
        "past_reads": normal_values(own_keys[11], (SEQS, CONV_TAPS - 1, GROUPS * STATE_DIM), 1.0, 6.0, ((0, 8),)),
        "step_bias": jnp.clip(jax.random.uniform(key_of[12], (HEADS,), jnp.float32, -4.0, -1.0), -4.0, -1.0),
        "decay_log": jnp.clip(jax.random.uniform(key_of[13], (HEADS,), jnp.float32, 0.0, 2.77), 0.0, 2.77),
        "skip_scale": jnp.clip(jnp.exp(jax.random.uniform(key_of[14], (HEADS,), jnp.float32, math.log(0.5), math.log(2.0))), 0.5, 2.0),
        "state_past": normal_values(own_keys[15], (SEQS, HEADS, HEAD_DIM, STATE_DIM), 0.5, 3.0, ((0, 8),), jnp.float32),
        "mixer_gain": jnp.clip(1.0 + 0.18 * jax.random.normal(key_of[16], (INNER,), jnp.float32), 0.1, 1.9),
        "out_weight": normal_values(key_of[17], (INNER, D), INNER ** -0.5, 0.125, ((1, 8),)),
        "norm1_gain": draw_norm1_gain(jax.random.fold_in(key_of[22], 71), part),
        "up_weight": normal_values(key_of[19], (D, FF), D ** -0.5, 0.09375, ((1, 8),)),
        "down_weight": gaussian_with(key_of[20], (FF, D), FF ** -0.5, 0.0625, ((0, 8),), (0, 1, 8, 2.0)),
        "norm2_gain": jnp.clip(1.0 + 0.18 * jax.random.normal(key_of[21], (D,), jnp.float32), 0.1, 1.9),
    }


RESIDUAL_SCALE = 2.0 ** 0.25
NORM_EPSILON = 1e-05
MIXER_EPSILON = 1e-06

def conv_silu(current, earlier, kernel):
    stacked = jnp.concatenate([earlier, current[:, None, :]], 1).astype(jnp.float32)
    return jax.nn.silu(lax.optimization_barrier(jnp.sum(stacked * kernel.astype(jnp.float32)[None], 1)))

def mixer_step(gate, values, writes, reads, steps, value_taps, write_taps, read_taps, past_values, past_writes, past_reads, step_bias, decay_log, skip_scale, state_past, mixer_gain):
    seq_count = gate.shape[0]
    values_act = conv_silu(values, past_values, value_taps).reshape(seq_count, HEADS, HEAD_DIM)
    writes_act = conv_silu(writes, past_writes, write_taps).reshape(seq_count, GROUPS, STATE_DIM)
    reads_act = conv_silu(reads, past_reads, read_taps).reshape(seq_count, GROUPS, STATE_DIM)
    per_group = HEADS // GROUPS
    writes_head = jnp.repeat(writes_act, per_group, axis=1)
    reads_head = jnp.repeat(reads_act, per_group, axis=1)
    step_size = jax.nn.softplus(steps.astype(jnp.float32) + step_bias)
    decays = jnp.exp(-step_size * jnp.exp(decay_log))
    state_next = decays[:, :, None, None] * state_past + (step_size[:, :, None] * values_act)[:, :, :, None] * writes_head[:, :, None, :]
    readout = jnp.einsum('shpn,shn->shp', state_next, reads_head, precision=lax.Precision.HIGHEST)
    readout = readout + skip_scale[None, :, None] * values_act
    gated = readout.reshape(seq_count, HEADS * HEAD_DIM) * jax.nn.silu(gate.astype(jnp.float32))
    grouped = gated.reshape(seq_count, GROUPS, -1)
    grouped = grouped * lax.rsqrt(lax.optimization_barrier(jnp.mean(jnp.square(grouped), -1, keepdims=True)) + MIXER_EPSILON)
    mixed = (grouped.reshape(seq_count, -1) * mixer_gain).astype(jnp.bfloat16)
    return (mixed, state_next)

def layer_norm(rows, gain):
    average = lax.optimization_barrier(jnp.mean(rows, -1, keepdims=True))
    variance = lax.optimization_barrier(jnp.mean(jnp.square(rows - average), -1, keepdims=True))
    return (rows - average) * lax.rsqrt(variance + NORM_EPSILON) * gain

def reference(layer_input, gate_weight, value_weight, write_weight, read_weight, step_weight, value_taps, write_taps, read_taps, past_values, past_writes, past_reads, step_bias, decay_log, skip_scale, state_past, mixer_gain, out_weight, norm1_gain, up_weight, down_weight, norm2_gain):

    def project(weight):
        return jnp.dot(layer_input, weight, preferred_element_type=jnp.float32).astype(jnp.bfloat16)
    gate = project(gate_weight)
    values = project(value_weight)
    writes = project(write_weight)
    reads = project(read_weight)
    steps = project(step_weight)
    mixed, state_next = mixer_step(gate, values, writes, reads, steps, value_taps, write_taps, read_taps, past_values, past_writes, past_reads, step_bias, decay_log, skip_scale, state_past, mixer_gain)
    mix_out = jnp.dot(mixed, out_weight, preferred_element_type=jnp.float32).astype(jnp.bfloat16)
    residual = RESIDUAL_SCALE * layer_input.astype(jnp.float32) + mix_out.astype(jnp.float32)
    normed = layer_norm(residual, norm1_gain).astype(jnp.bfloat16)
    hidden = jnp.square(jax.nn.relu(jnp.dot(normed, up_weight, preferred_element_type=jnp.float32))).astype(jnp.bfloat16)
    channel = jnp.dot(hidden, down_weight, preferred_element_type=jnp.float32).astype(jnp.bfloat16)
    second = RESIDUAL_SCALE * normed.astype(jnp.float32) + channel.astype(jnp.float32)
    layer_output = layer_norm(second, norm2_gain).astype(jnp.bfloat16)
    return (layer_output, state_next)
```

```python
import functools

import jax
import jax.numpy as jnp
from jax import lax
from jax.experimental import pallas as pl
from jax.experimental.pallas import tpu as pltpu
from jax.sharding import PartitionSpec as P

HEADS = 32
HEAD_DIM = 64
STATE_DIM = 128
GROUPS = 2

RESIDUAL_SCALE = 2.0**0.25
NORM_EPSILON = 1e-05
MIXER_EPSILON = 1e-06

F32 = jnp.float32
BF16 = jnp.bfloat16
ANY = pl.BlockSpec(memory_space=pl.ANY)
VMEM = pl.BlockSpec(memory_space=pltpu.VMEM)


def silu(v):
    return v * jax.nn.sigmoid(v)


def layer_kernel(geo, *refs):
    n, tp_size, seqs, rows, width, offsets, ways, halves = geo
    inputs = refs[:22]
    layer_out, decay_out, drive_out, write_out = refs[22:26]
    held = refs[26:48]
    (
        wide, send1, recv1, spread, read_out, mix_all, mix_rows, res_all, normed_f, own_normed,
        normed_b, hidden, down_rows, send2, recv2, finished, done_all, done_rows,
        load_sem, s1, r1, s2, r2, s3, r3, s4, r4, s5, r5,
    ) = refs[48:]
    (
        x, gate_w, value_w, write_w, read_w, step_w, value_taps, write_taps, read_taps, past_values,
        past_writes, past_reads, step_bias, decay_log, skip_scale, state, mixer_gain, out_w, gain1,
        up_w, down_w, gain2,
    ) = held
    inner = value_w.shape[1]
    model = gain1.shape[1]
    cols = x.shape[1]
    me = lax.axis_index("kv") * tp_size + lax.axis_index("tp")

    def peer(step):
        other = lax.rem(me + step, n)
        return other, {"kv": lax.div(other, tp_size), "tp": lax.rem(other, tp_size)}

    loads = {}
    count = 0
    for i in range(22):
        parts = ways if i in (19, 20) else 1
        depth = inputs[i].shape[0] // parts
        loads[i] = []
        for part in range(parts):
            if parts == 1:
                src, dst = inputs[i], held[i]
            else:
                src = inputs[i].at[pl.ds(part * depth, depth)]
                dst = held[i].at[pl.ds(part * depth, depth)]
            loads[i].append(pltpu.make_async_copy(src, dst, load_sem.at[count]))
            count += 1

    def start(*which):
        for i in which:
            for copy in loads[i]:
                copy.start()

    def wait(*which):
        for i in which:
            for copy in loads[i]:
                copy.wait()

    start(0, 5, 3, 4, 2, 1)
    start(6, 7, 8, 9, 10, 11, 12, 13, 14, 16, 18, 21)
    start(15)

    barrier = pltpu.get_barrier_semaphore()
    for j in range(1, n):
        pl.semaphore_signal(
            barrier, inc=1, device_id=peer(j)[1], device_id_type=pl.DeviceIdType.MESH
        )

    def exchange(source, target, send_sem, recv_sem):
        copies = []
        for j in range(1, n):
            other, where = peer(j)
            copy = pltpu.make_async_remote_copy(
                src_ref=source(other),
                dst_ref=target(j),
                send_sem=send_sem.at[j],
                recv_sem=recv_sem.at[j],
                device_id=where,
                device_id_type=pl.DeviceIdType.MESH,
            )
            copy.start()
            copies.append(copy)
        return copies

    wait(0)
    wide[:, offsets[4] :] = jnp.zeros((rows, width - offsets[4]), F32)
    order = (5, 3, 4, 2, 1)
    for place, i in enumerate(order):
        wait(i)
        if place == len(order) - 1:
            start(17, 19, 20)
        w = held[i]
        for begin in range(0, w.shape[1], 512):
            size = min(512, w.shape[1] - begin)
            wide[:, offsets[i - 1] + begin : offsets[i - 1] + begin + size] = jnp.dot(
                x[...], w[:, begin : begin + size], preferred_element_type=F32
            )
    for d in range(n):
        send1[d] = wide[d * seqs : (d + 1) * seqs, :].astype(BF16)
    pl.semaphore_wait(barrier, n - 1)
    first = exchange(lambda other: send1.at[other], lambda j: recv1.at[j], s1, r1)

    wait(6, 7, 8, 9, 10, 11, 12, 13, 14, 16, 18, 21, 15)
    head_of = lax.broadcasted_iota(jnp.int32, (HEADS, inner), 1) // HEAD_DIM
    spreader = (head_of == lax.broadcasted_iota(jnp.int32, (HEADS, inner), 0)).astype(F32)

    total = send1[me].astype(F32)
    for j in range(1, n):
        first[j - 1].wait_recv()
        total = total + recv1[j].astype(F32)
    total = total.astype(BF16).astype(F32)

    def conv(now, past, taps):
        t = taps[...].astype(F32)
        p = past[...].astype(F32)
        acc = now * t[3:4]
        for k in range(3):
            acc = acc + p[:, k, :] * t[k : k + 1]
        return silu(acc)

    groups = GROUPS * STATE_DIM
    gate = total[:, offsets[0] : offsets[0] + inner]
    values = conv(total[:, offsets[1] : offsets[1] + inner], past_values, value_taps)
    writes = conv(total[:, offsets[2] : offsets[2] + groups], past_writes, write_taps)
    reads = conv(total[:, offsets[3] : offsets[3] + groups], past_reads, read_taps)
    raw = total[:, offsets[4] : offsets[4] + HEADS] + step_bias[...]
    step_size = jnp.maximum(raw, 0.0) + jnp.log1p(jnp.exp(-jnp.abs(raw)))
    decays = jnp.exp(-step_size * jnp.exp(decay_log[...]))
    pad = spread.shape[0] // 3
    spread[...] = jnp.zeros(spread.shape, F32)
    spread[0:seqs, :] = step_size
    spread[pad : pad + seqs, :] = decays
    spread[2 * pad : 2 * pad + 1, :] = skip_scale[...]
    per_channel = jnp.dot(
        spread[...], spreader, preferred_element_type=F32, precision=lax.Precision.HIGHEST
    )
    step_c = per_channel[0:seqs]
    decay_c = per_channel[pad : pad + seqs]
    skip_c = per_channel[2 * pad : 2 * pad + 1]
    half = inner // GROUPS
    for g in range(GROUPS):
        reads_g = reads[:, g * STATE_DIM : (g + 1) * STATE_DIM].astype(BF16)
        for s in range(seqs):
            block = state[s, g * half : (g + 1) * half, :].astype(BF16)
            seen = lax.dot_general(
                reads_g, block, (((1,), (1,)), ((), ())), preferred_element_type=F32
            )
            read_out[s : s + 1, g * half : (g + 1) * half] = seen[s : s + 1]
    drive = step_c * values
    decay_out[...] = jnp.zeros(decay_out.shape, F32)
    drive_out[...] = jnp.zeros(drive_out.shape, F32)
    write_out[...] = jnp.zeros(write_out.shape, F32)
    decay_out[0:seqs, :] = decay_c
    drive_out[0:seqs, :] = drive
    write_out[0:seqs, :] = writes
    base = decay_c * read_out[...] + skip_c * values
    gate_act = silu(gate)
    product = writes * reads
    for g in range(GROUPS):
        here = slice(g * half, (g + 1) * half)
        overlap = jnp.sum(product[:, g * STATE_DIM : (g + 1) * STATE_DIM], -1, keepdims=True)
        gated = (base[:, here] + drive[:, here] * overlap) * gate_act[:, here]
        scale = lax.rsqrt(jnp.mean(gated * gated, -1, keepdims=True) + MIXER_EPSILON)
        mix_all[me, :, here] = (gated * scale * mixer_gain[:, here]).astype(BF16)
    second = exchange(lambda other: mix_all.at[me], lambda j: mix_all.at[me], s2, r2)

    wait(17)
    for copy in second:
        copy.wait_recv()
    for d in range(n):
        mix_rows[d * seqs : (d + 1) * seqs, :] = mix_all[d].astype(F32)
    mix_out = jnp.dot(mix_rows[...].astype(BF16), out_w[...], preferred_element_type=F32)
    residual = RESIDUAL_SCALE * x[...].astype(F32) + mix_out.astype(BF16).astype(F32)
    res_all[me] = residual.astype(BF16)
    third = exchange(lambda other: res_all.at[me], lambda j: res_all.at[me], s3, r3)

    wait(19, 20)
    for copy in third:
        copy.wait_recv()
    total1 = jnp.zeros((rows, 1), F32)
    for d in range(n):
        total1 = total1 + jnp.sum(res_all[d].astype(F32), -1, keepdims=True)
    average = total1 / model
    total2 = jnp.zeros((rows, 1), F32)
    for d in range(n):
        off = res_all[d].astype(F32) - average
        total2 = total2 + jnp.sum(off * off, -1, keepdims=True)
    scale = lax.rsqrt(total2 / model + NORM_EPSILON)
    for d in range(n):
        here = slice(d * cols, (d + 1) * cols)
        block = (res_all[d].astype(F32) - average) * scale * gain1[:, here]
        normed_b[:, here] = block.astype(BF16)
        normed_f[:, here] = block.astype(BF16).astype(F32)
    for d in range(n):

        @pl.when(me == d)
        def _():
            own_normed[...] = normed_f[d * seqs : (d + 1) * seqs, :]

    chunk = min(256, up_w.shape[1])

    @pl.loop(0, up_w.shape[1] // chunk)
    def _(c):
        here = pl.ds(pl.multiple_of(c * chunk, chunk), chunk)
        h = jnp.dot(normed_b[...], up_w[:, here], preferred_element_type=F32)
        h = jnp.maximum(h, 0.0)
        hidden[:, here] = (h * h).astype(BF16)

    span = model // halves
    fourth = []
    for part in range(halves):

        @pl.loop(0, span // 512)
        def _(c):
            there = pl.ds(pl.multiple_of(c * 512, 512), 512)
            here = pl.ds(pl.multiple_of(part * span + c * 512, 512), 512)
            down_rows[:, there] = jnp.dot(
                hidden[...], down_w[:, here], preferred_element_type=F32
            )

        for d in range(n):
            send2[part, d] = down_rows[d * seqs : (d + 1) * seqs, :].astype(BF16)
        fourth.append(
            exchange(
                lambda other: send2.at[part, other],
                lambda j: recv2.at[part, j],
                s4.at[part],
                r4.at[part],
            )
        )

    rows2 = []
    for part in range(halves):
        channel = send2[part, me].astype(F32)
        for j in range(1, n):
            fourth[part][j - 1].wait_recv()
            channel = channel + recv2[part, j].astype(F32)
        rows2.append(
            RESIDUAL_SCALE * own_normed[:, part * span : (part + 1) * span]
            + channel.astype(BF16).astype(F32)
        )
    average = sum(jnp.sum(r, -1, keepdims=True) for r in rows2) / model
    rows2 = [r - average for r in rows2]
    variance = sum(jnp.sum(r * r, -1, keepdims=True) for r in rows2) / model
    scale = lax.rsqrt(variance + NORM_EPSILON)
    for d in range(n):
        part, begin = divmod(d * cols, span)
        block = rows2[part][:, begin : begin + cols] * scale * gain2[:, d * cols : (d + 1) * cols]
        finished[d] = block.astype(BF16)
    done_all[me] = finished[me]
    fifth = exchange(lambda other: finished.at[other], lambda j: done_all.at[me], s5, r5)
    for copy in fifth:
        copy.wait_recv()
    for d in range(n):
        done_rows[d * seqs : (d + 1) * seqs, :] = done_all[d].astype(F32)
    layer_out[...] = done_rows[...].astype(BF16)
    for group in [first, second, third, *fourth, fifth]:
        for copy in group:
            copy.wait_send()


def state_kernel(seqs, state, decay, drive, write, layer_in, state_out, layer_out):
    decay_t = jnp.transpose(decay[...])
    drive_t = jnp.transpose(drive[...])
    for s in range(seqs):
        state_out[s] = decay_t[:, s : s + 1] * state[s] + drive_t[:, s : s + 1] * write[s : s + 1, :]
    layer_out[...] = layer_in[...]


def on_device(n, tp_size, *args):
    x = args[0]
    state = args[15]
    seqs, rows, cols = state.shape[0], x.shape[0], x.shape[1]
    inner = args[1].shape[1]
    model = args[18].shape[0]
    hidden_here = args[19].shape[1]
    offsets = [0]
    for i in range(1, 5):
        offsets.append(offsets[-1] + args[i].shape[1])
    width = offsets[-1] + 128
    args = list(args)
    args[15] = state.reshape(seqs, inner, STATE_DIM)
    for i in (12, 13, 14, 16, 18, 21):
        args[i] = args[i].reshape(1, -1)
    ways, halves = 4, 2
    pad = (seqs + 7) // 8 * 8
    dma = pltpu.SemaphoreType.DMA
    scratch = [pltpu.VMEM(a.shape, a.dtype) for a in args]
    scratch += [
        pltpu.VMEM((rows, width), F32),
        pltpu.VMEM((n, seqs, width), BF16),
        pltpu.VMEM((n, seqs, width), BF16),
        pltpu.VMEM((3 * pad, HEADS), F32),
        pltpu.VMEM((seqs, inner), F32),
        pltpu.VMEM((n, seqs, inner), BF16),
        pltpu.VMEM((rows, inner), F32),
        pltpu.VMEM((n, rows, cols), BF16),
        pltpu.VMEM((rows, model), F32),
        pltpu.VMEM((seqs, model), F32),
        pltpu.VMEM((rows, model), BF16),
        pltpu.VMEM((rows, hidden_here), BF16),
        pltpu.VMEM((rows, model // halves), F32),
        pltpu.VMEM((halves, n, seqs, model // halves), BF16),
        pltpu.VMEM((halves, n, seqs, model // halves), BF16),
        pltpu.VMEM((n, seqs, cols), BF16),
        pltpu.VMEM((n, seqs, cols), BF16),
        pltpu.VMEM((rows, cols), F32),
        dma((20 + 2 * ways,)),
        dma((n,)), dma((n,)), dma((n,)), dma((n,)), dma((n,)), dma((n,)),
        dma((halves, n)), dma((halves, n)), dma((n,)), dma((n,)),
    ]
    geo = (n, tp_size, seqs, rows, width, tuple(offsets), ways, halves)
    layer_rows, decay, drive, write = pl.pallas_call(
        functools.partial(layer_kernel, geo),
        out_shape=(
            jax.ShapeDtypeStruct((rows, cols), BF16),
            jax.ShapeDtypeStruct((pad, inner), F32),
            jax.ShapeDtypeStruct((pad, inner), F32),
            jax.ShapeDtypeStruct((pad, GROUPS * STATE_DIM), F32),
        ),
        in_specs=[ANY] * 22,
        out_specs=(VMEM,) * 4,
        scratch_shapes=scratch,
        compiler_params=pltpu.CompilerParams(
            collective_id=0, has_side_effects=True, vmem_limit_bytes=60 * 1024 * 1024
        ),
        name="layer",
    )(*args)
    block = 256
    per_group = inner // GROUPS // block
    state_next, result = pl.pallas_call(
        functools.partial(state_kernel, seqs),
        grid=(inner // block,),
        in_specs=[
            pl.BlockSpec((seqs, block, STATE_DIM), lambda i: (0, i, 0)),
            pl.BlockSpec((pad, block), lambda i: (0, i)),
            pl.BlockSpec((pad, block), lambda i: (0, i)),
            pl.BlockSpec((pad, STATE_DIM), lambda i: (0, i // per_group)),
            pl.BlockSpec((rows, cols), lambda i: (0, 0)),
        ],
        out_specs=(
            pl.BlockSpec((seqs, block, STATE_DIM), lambda i: (0, i, 0)),
            pl.BlockSpec((rows, cols), lambda i: (0, 0)),
        ),
        out_shape=(
            jax.ShapeDtypeStruct((seqs, inner, STATE_DIM), F32),
            jax.ShapeDtypeStruct((rows, cols), BF16),
        ),
        name="state",
    )(args[15], decay, drive, write, layer_rows)
    return result, state_next.reshape(state.shape)


def solution(mesh):
    tp_size = mesh.shape["tp"]
    n = mesh.shape["kv"] * tp_size
    split, whole = P(("kv", "tp"), None), P()
    past = P(("dp", "kv", "tp"), None, None)
    states = P(("dp", "kv", "tp"), None, None, None)
    columns = P(None, ("kv", "tp"))
    placed = (
        (P("dp", ("kv", "tp")),) + (split,) * 5 + (whole,) * 3 + (past,) * 3 + (whole,) * 3
        + (states, whole, columns, whole, columns, split, whole)
    )
    return jax.shard_map(
        functools.partial(on_device, n, tp_size),
        mesh=mesh,
        in_specs=placed,
        out_specs=(P("dp", ("kv", "tp")), states),
        check_vma=False,
    )
```

```python
import functools

import jax
import jax.numpy as jnp
from jax import lax
from jax.experimental import pallas as pl
from jax.experimental.pallas import tpu as pltpu
from jax.sharding import PartitionSpec as P

HEADS = 32
HEAD_DIM = 64
STATE_DIM = 128
GROUPS = 2

RESIDUAL_SCALE = 2.0**0.25
NORM_EPSILON = 1e-05
MIXER_EPSILON = 1e-06

F32 = jnp.float32
BF16 = jnp.bfloat16
ANY = pl.BlockSpec(memory_space=pl.ANY)
VMEM = pl.BlockSpec(memory_space=pltpu.VMEM)


def silu(v):
    return v * jax.nn.sigmoid(v)


def layer_kernel(geo, *refs):
    n, tp_size, seqs, rows, width, offsets, ways, halves = geo
    inputs = refs[:22]
    layer_out, state_out = refs[22:24]
    held = refs[24:46]
    decay_out, drive_out, write_out = refs[46:49]
    (
        wide, send1, recv1, spread, read_out, mix_all, mix_rows, res_all, normed_f, own_normed,
        normed_b, hidden, down_rows, send2, recv2, finished, done_all, done_rows,
        load_sem, store_sem, s1, r1, s2, r2, s3, r3, s4, r4, s5, r5,
    ) = refs[49:]
    (
        x, gate_w, value_w, write_w, read_w, step_w, value_taps, write_taps, read_taps, past_values,
        past_writes, past_reads, step_bias, decay_log, skip_scale, state, mixer_gain, out_w, gain1,
        up_w, down_w, gain2,
    ) = held
    inner = value_w.shape[1]
    model = gain1.shape[1]
    cols = x.shape[1]
    me = lax.axis_index("kv") * tp_size + lax.axis_index("tp")

    def peer(step):
        other = lax.rem(me + step, n)
        return other, {"kv": lax.div(other, tp_size), "tp": lax.rem(other, tp_size)}

    loads = {}
    count = 0
    for i in range(22):
        parts = ways if i in (19, 20) else 1
        depth = inputs[i].shape[0] // parts
        loads[i] = []
        for part in range(parts):
            if parts == 1:
                src, dst = inputs[i], held[i]
            else:
                src = inputs[i].at[pl.ds(part * depth, depth)]
                dst = held[i].at[pl.ds(part * depth, depth)]
            loads[i].append(pltpu.make_async_copy(src, dst, load_sem.at[count]))
            count += 1

    def start(*which):
        for i in which:
            for copy in loads[i]:
                copy.start()

    def wait(*which):
        for i in which:
            for copy in loads[i]:
                copy.wait()

    start(0, 5, 3, 4, 2, 1)
    start(6, 7, 8, 9, 10, 11, 12, 13, 14, 16, 18, 21)
    start(15)

    barrier = pltpu.get_barrier_semaphore()
    for j in range(1, n):
        pl.semaphore_signal(
            barrier, inc=1, device_id=peer(j)[1], device_id_type=pl.DeviceIdType.MESH
        )

    def exchange(source, target, send_sem, recv_sem):
        copies = []
        for j in range(1, n):
            other, where = peer(j)
            copy = pltpu.make_async_remote_copy(
                src_ref=source(other),
                dst_ref=target(j),
                send_sem=send_sem.at[j],
                recv_sem=recv_sem.at[j],
                device_id=where,
                device_id_type=pl.DeviceIdType.MESH,
            )
            copy.start()
            copies.append(copy)
        return copies

    wait(0)
    wide[:, offsets[4] :] = jnp.zeros((rows, width - offsets[4]), F32)
    order = (5, 3, 4, 2, 1)
    for place, i in enumerate(order):
        wait(i)
        if place == len(order) - 1:
            start(17, 19, 20)
        w = held[i]
        if i == 5:
            wide[:, offsets[4] : offsets[4] + HEADS] = lax.dot_general(
                x[...], w[...], (((1,), (1,)), ((), ())), preferred_element_type=F32
            )
            continue
        for begin in range(0, w.shape[1], 512):
            size = min(512, w.shape[1] - begin)
            wide[:, offsets[i - 1] + begin : offsets[i - 1] + begin + size] = jnp.dot(
                x[...], w[:, begin : begin + size], preferred_element_type=F32
            )
    for d in range(n):
        send1[d] = wide[d * seqs : (d + 1) * seqs, :].astype(BF16)
    pl.semaphore_wait(barrier, n - 1)
    first = exchange(lambda other: send1.at[other], lambda j: recv1.at[j], s1, r1)

    wait(6, 7, 8, 9, 10, 11, 12, 13, 14, 16, 18, 21, 15)
    head_of = lax.broadcasted_iota(jnp.int32, (HEADS, inner), 1) // HEAD_DIM
    spreader = (head_of == lax.broadcasted_iota(jnp.int32, (HEADS, inner), 0)).astype(F32)

    total = send1[me].astype(F32)
    for j in range(1, n):
        first[j - 1].wait_recv()
        total = total + recv1[j].astype(F32)
    total = total.astype(BF16).astype(F32)

    def conv(now, past, taps):
        t = taps[...].astype(F32)
        p = past[...].astype(F32)
        acc = now * t[3:4]
        for k in range(3):
            acc = acc + p[k] * t[k : k + 1]
        return silu(acc)

    groups = GROUPS * STATE_DIM
    gate = total[:, offsets[0] : offsets[0] + inner]
    values = conv(total[:, offsets[1] : offsets[1] + inner], past_values, value_taps)
    writes = conv(total[:, offsets[2] : offsets[2] + groups], past_writes, write_taps)
    reads = conv(total[:, offsets[3] : offsets[3] + groups], past_reads, read_taps)
    raw = total[:, offsets[4] : offsets[4] + HEADS] + step_bias[...]
    step_size = jnp.maximum(raw, 0.0) + jnp.log1p(jnp.exp(-jnp.abs(raw)))
    decays = jnp.exp(-step_size * jnp.exp(decay_log[...]))
    pad = spread.shape[0] // 3
    spread[...] = jnp.zeros(spread.shape, F32)
    spread[0:seqs, :] = step_size
    spread[pad : pad + seqs, :] = decays
    spread[2 * pad : 2 * pad + 1, :] = skip_scale[...]
    per_channel = jnp.dot(
        spread[...], spreader, preferred_element_type=F32, precision=lax.Precision.HIGHEST
    )
    step_c = per_channel[0:seqs]
    decay_c = per_channel[pad : pad + seqs]
    skip_c = per_channel[2 * pad : 2 * pad + 1]
    half = inner // GROUPS
    for g in range(GROUPS):
        reads_g = reads[:, g * STATE_DIM : (g + 1) * STATE_DIM].astype(BF16)
        for s in range(seqs):
            block = state[s, g * half : (g + 1) * half, :].astype(BF16)
            seen = lax.dot_general(
                reads_g, block, (((1,), (1,)), ((), ())), preferred_element_type=F32
            )
            read_out[s : s + 1, g * half : (g + 1) * half] = seen[s : s + 1]
    drive = step_c * values
    decay_out[...] = jnp.zeros(decay_out.shape, F32)
    drive_out[...] = jnp.zeros(drive_out.shape, F32)
    write_out[...] = jnp.zeros(write_out.shape, F32)
    decay_out[0:seqs, :] = decay_c
    drive_out[0:seqs, :] = drive
    write_out[0:seqs, :] = writes
    base = decay_c * read_out[...] + skip_c * values
    gate_act = silu(gate)
    product = writes * reads
    for g in range(GROUPS):
        here = slice(g * half, (g + 1) * half)
        overlap = jnp.sum(product[:, g * STATE_DIM : (g + 1) * STATE_DIM], -1, keepdims=True)
        gated = (base[:, here] + drive[:, here] * overlap) * gate_act[:, here]
        scale = lax.rsqrt(jnp.mean(gated * gated, -1, keepdims=True) + MIXER_EPSILON)
        mix_all[me, :, here] = (gated * scale * mixer_gain[:, here]).astype(BF16)
    second = exchange(lambda other: mix_all.at[me], lambda j: mix_all.at[me], s2, r2)

    strip = 256
    stores = []

    def update_states(g):
        @pl.loop(0, half // strip)
        def _(b):
            here = pl.ds(pl.multiple_of(g * half + b * strip, strip), strip)
            decay_t = jnp.transpose(decay_out[:, here])
            drive_t = jnp.transpose(drive_out[:, here])
            for s in range(seqs):
                write = write_out[s : s + 1, g * STATE_DIM : (g + 1) * STATE_DIM]
                state[s, here, :] = (
                    decay_t[:, s : s + 1] * state[s, here, :] + drive_t[:, s : s + 1] * write
                )

        where = pl.ds(g * half, half)
        store = pltpu.make_async_copy(
            state.at[:, where], state_out.at[:, where], store_sem.at[g]
        )
        store.start()
        stores.append(store)

    update_states(0)

    wait(17)
    for copy in second:
        copy.wait_recv()
    for d in range(n):
        mix_rows[d * seqs : (d + 1) * seqs, :] = mix_all[d].astype(F32)
    mix_out = jnp.dot(mix_rows[...].astype(BF16), out_w[...], preferred_element_type=F32)
    residual = RESIDUAL_SCALE * x[...].astype(F32) + mix_out.astype(BF16).astype(F32)
    res_all[me] = residual.astype(BF16)
    third = exchange(lambda other: res_all.at[me], lambda j: res_all.at[me], s3, r3)
    for g in range(1, GROUPS):
        update_states(g)

    wait(19, 20)
    for copy in third:
        copy.wait_recv()
    total1 = jnp.zeros((rows, 1), F32)
    for d in range(n):
        total1 = total1 + jnp.sum(res_all[d].astype(F32), -1, keepdims=True)
    average = total1 / model
    total2 = jnp.zeros((rows, 1), F32)
    for d in range(n):
        off = res_all[d].astype(F32) - average
        total2 = total2 + jnp.sum(off * off, -1, keepdims=True)
    scale = lax.rsqrt(total2 / model + NORM_EPSILON)
    for d in range(n):
        here = slice(d * cols, (d + 1) * cols)
        block = (res_all[d].astype(F32) - average) * scale * gain1[:, here]
        normed_b[:, here] = block.astype(BF16)
        normed_f[:, here] = block.astype(BF16).astype(F32)
    for d in range(n):

        @pl.when(me == d)
        def _():
            own_normed[...] = normed_f[d * seqs : (d + 1) * seqs, :]

    chunk = min(256, up_w.shape[1])

    @pl.loop(0, up_w.shape[1] // chunk)
    def _(c):
        here = pl.ds(pl.multiple_of(c * chunk, chunk), chunk)
        h = jnp.dot(normed_b[...], up_w[:, here], preferred_element_type=F32)
        h = jnp.maximum(h, 0.0)
        hidden[:, here] = (h * h).astype(BF16)

    span = model // halves
    fourth = []
    for part in range(halves):

        @pl.loop(0, span // 512)
        def _(c):
            there = pl.ds(pl.multiple_of(c * 512, 512), 512)
            here = pl.ds(pl.multiple_of(part * span + c * 512, 512), 512)
            down_rows[:, there] = jnp.dot(
                hidden[...], down_w[:, here], preferred_element_type=F32
            )

        for d in range(n):
            send2[part, d] = down_rows[d * seqs : (d + 1) * seqs, :].astype(BF16)
        fourth.append(
            exchange(
                lambda other: send2.at[part, other],
                lambda j: recv2.at[part, j],
                s4.at[part],
                r4.at[part],
            )
        )

    rows2 = []
    for part in range(halves):
        channel = send2[part, me].astype(F32)
        for j in range(1, n):
            fourth[part][j - 1].wait_recv()
            channel = channel + recv2[part, j].astype(F32)
        rows2.append(
            RESIDUAL_SCALE * own_normed[:, part * span : (part + 1) * span]
            + channel.astype(BF16).astype(F32)
        )
    average = sum(jnp.sum(r, -1, keepdims=True) for r in rows2) / model
    rows2 = [r - average for r in rows2]
    variance = sum(jnp.sum(r * r, -1, keepdims=True) for r in rows2) / model
    scale = lax.rsqrt(variance + NORM_EPSILON)
    for d in range(n):
        part, begin = divmod(d * cols, span)
        block = rows2[part][:, begin : begin + cols] * scale * gain2[:, d * cols : (d + 1) * cols]
        finished[d] = block.astype(BF16)
    done_all[me] = finished[me]
    fifth = exchange(lambda other: finished.at[other], lambda j: done_all.at[me], s5, r5)
    for copy in fifth:
        copy.wait_recv()
    for d in range(n):
        done_rows[d * seqs : (d + 1) * seqs, :] = done_all[d].astype(F32)
    layer_out[...] = done_rows[...].astype(BF16)
    for store in stores:
        store.wait()
    for group in [first, second, third, *fourth, fifth]:
        for copy in group:
            copy.wait_send()


def on_device(n, tp_size, *args):
    x = args[0]
    state = args[15]
    seqs, rows, cols = state.shape[0], x.shape[0], x.shape[1]
    inner = args[1].shape[1]
    model = args[18].shape[0]
    hidden_here = args[19].shape[1]
    offsets = [0]
    for i in range(1, 5):
        offsets.append(offsets[-1] + args[i].shape[1])
    width = offsets[-1] + 128
    args = list(args)
    args[15] = state.reshape(seqs, inner, STATE_DIM)
    args[5] = args[5].T
    for i in (9, 10, 11):
        args[i] = jnp.transpose(args[i], (1, 0, 2))
    for i in (12, 13, 14, 16, 18, 21):
        args[i] = args[i].reshape(1, -1)
    ways, halves = 4, 2
    pad = (seqs + 7) // 8 * 8
    dma = pltpu.SemaphoreType.DMA
    scratch = [pltpu.VMEM(a.shape, a.dtype) for a in args]
    scratch += [
        pltpu.VMEM((pad, inner), F32),
        pltpu.VMEM((pad, inner), F32),
        pltpu.VMEM((pad, GROUPS * STATE_DIM), F32),
        pltpu.VMEM((rows, width), F32),
        pltpu.VMEM((n, seqs, width), BF16),
        pltpu.VMEM((n, seqs, width), BF16),
        pltpu.VMEM((3 * pad, HEADS), F32),
        pltpu.VMEM((seqs, inner), F32),
        pltpu.VMEM((n, seqs, inner), BF16),
        pltpu.VMEM((rows, inner), F32),
        pltpu.VMEM((n, rows, cols), BF16),
        pltpu.VMEM((rows, model), F32),
        pltpu.VMEM((seqs, model), F32),
        pltpu.VMEM((rows, model), BF16),
        pltpu.VMEM((rows, hidden_here), BF16),
        pltpu.VMEM((rows, model // halves), F32),
        pltpu.VMEM((halves, n, seqs, model // halves), BF16),
        pltpu.VMEM((halves, n, seqs, model // halves), BF16),
        pltpu.VMEM((n, seqs, cols), BF16),
        pltpu.VMEM((n, seqs, cols), BF16),
        pltpu.VMEM((rows, cols), F32),
        dma((20 + 2 * ways,)),
        dma((GROUPS,)),
        dma((n,)), dma((n,)), dma((n,)), dma((n,)), dma((n,)), dma((n,)),
        dma((halves, n)), dma((halves, n)), dma((n,)), dma((n,)),
    ]
    geo = (n, tp_size, seqs, rows, width, tuple(offsets), ways, halves)
    result, state_next = pl.pallas_call(
        functools.partial(layer_kernel, geo),
        out_shape=(
            jax.ShapeDtypeStruct((rows, cols), BF16),
            jax.ShapeDtypeStruct((seqs, inner, STATE_DIM), F32),
        ),
        in_specs=[ANY] * 22,
        out_specs=(VMEM, ANY),
        scratch_shapes=scratch,
        compiler_params=pltpu.CompilerParams(
            collective_id=0, has_side_effects=True, vmem_limit_bytes=67043328
        ),
        name="layer",
    )(*args)
    return result, state_next.reshape(state.shape)


def solution(mesh):
    tp_size = mesh.shape["tp"]
    n = mesh.shape["kv"] * tp_size
    split, whole = P(("kv", "tp"), None), P()
    past = P(("dp", "kv", "tp"), None, None)
    states = P(("dp", "kv", "tp"), None, None, None)
    columns = P(None, ("kv", "tp"))
    placed = (
        (P("dp", ("kv", "tp")),) + (split,) * 5 + (whole,) * 3 + (past,) * 3 + (whole,) * 3
        + (states, whole, columns, whole, columns, split, whole)
    )
    return jax.shard_map(
        functools.partial(on_device, n, tp_size),
        mesh=mesh,
        in_specs=placed,
        out_specs=(P("dp", ("kv", "tp")), states),
        check_vma=False,
    )
```

```python
import functools

import jax
import jax.numpy as jnp
from jax import lax
from jax.experimental import pallas as pl
from jax.experimental.pallas import tpu as pltpu
from jax.sharding import PartitionSpec as P

HEADS = 32
HEAD_DIM = 64
STATE_DIM = 128
GROUPS = 2

RESIDUAL_SCALE = 2.0**0.25
NORM_EPSILON = 1e-05
MIXER_EPSILON = 1e-06

F32 = jnp.float32
BF16 = jnp.bfloat16
ANY = pl.BlockSpec(memory_space=pl.ANY)
VMEM = pl.BlockSpec(memory_space=pltpu.VMEM)


def silu(v):
    return v * jax.nn.sigmoid(v)


def layer_kernel(geo, *refs):
    n, tp_size, seqs, rows, width, offsets, ways, halves = geo
    inputs = refs[:22]
    layer_out, state_out = refs[22:24]
    held = refs[24:46]
    decay_out, drive_out, write_out = refs[46:49]
    (
        wide, send1, recv1, send_gate, recv_gate, spread, read_out, mix_all, mix_rows, res_all, normed_f, own_normed,
        normed_b, hidden, down_rows, send2, recv2, finished, done_all, done_rows,
        load_sem, store_sem, s1, r1, s2, r2, s3, r3, s4, r4, s5, r5, s6, r6,
        s7, r7,
    ) = refs[49:]
    (
        x, gate_w, value_w, write_w, read_w, step_w, value_taps, write_taps, read_taps, past_values,
        past_writes, past_reads, step_bias, decay_log, skip_scale, state, mixer_gain, out_w, gain1,
        up_w, down_w, gain2,
    ) = held
    inner = value_w.shape[1]
    model = gain1.shape[1]
    cols = x.shape[1]
    me = lax.axis_index("kv") * tp_size + lax.axis_index("tp")

    def peer(step):
        other = lax.rem(me + step, n)
        return other, {"kv": lax.div(other, tp_size), "tp": lax.rem(other, tp_size)}

    loads = {}
    count = 0
    for i in range(22):
        parts = ways if i in (19, 20) else 1
        depth = inputs[i].shape[0] // parts
        loads[i] = []
        for part in range(parts):
            if parts == 1:
                src, dst = inputs[i], held[i]
            else:
                src = inputs[i].at[pl.ds(part * depth, depth)]
                dst = held[i].at[pl.ds(part * depth, depth)]
            loads[i].append(pltpu.make_async_copy(src, dst, load_sem.at[count]))
            count += 1

    def start(*which):
        for i in which:
            for copy in loads[i]:
                copy.start()

    def wait(*which):
        for i in which:
            for copy in loads[i]:
                copy.wait()

    start(0, 5, 3, 4, 2, 1)
    start(6, 7, 8, 9, 10, 11, 12, 13, 14, 16, 18, 21)
    start(15)

    barrier = pltpu.get_barrier_semaphore()
    for j in range(1, n):
        pl.semaphore_signal(
            barrier, inc=1, device_id=peer(j)[1], device_id_type=pl.DeviceIdType.MESH
        )

    def exchange(source, target, send_sem, recv_sem):
        copies = []
        for j in range(1, n):
            other, where = peer(j)
            copy = pltpu.make_async_remote_copy(
                src_ref=source(other),
                dst_ref=target(j),
                send_sem=send_sem.at[j],
                recv_sem=recv_sem.at[j],
                device_id=where,
                device_id_type=pl.DeviceIdType.MESH,
            )
            copy.start()
            copies.append(copy)
        return copies

    wait(0)
    wide[:, offsets[4] :] = jnp.zeros((rows, width - offsets[4]), F32)
    order = (5, 3, 4, 2, 1)
    for place, i in enumerate(order):
        wait(i)
        if place == len(order) - 1:
            start(17, 19, 20)
            for d in range(n):
                send1[d] = wide[d * seqs : (d + 1) * seqs, inner:].astype(BF16)
            pl.semaphore_wait(barrier, n - 1)
            first = exchange(lambda other: send1.at[other], lambda j: recv1.at[j], s1, r1)
        w = held[i]
        if i == 5:
            wide[:, offsets[4] : offsets[4] + HEADS] = lax.dot_general(
                x[...], w[...], (((1,), (1,)), ((), ())), preferred_element_type=F32
            )
            continue
        for begin in range(0, w.shape[1], 512):
            size = min(512, w.shape[1] - begin)
            wide[:, offsets[i - 1] + begin : offsets[i - 1] + begin + size] = jnp.dot(
                x[...], w[:, begin : begin + size], preferred_element_type=F32
            )
    for d in range(n):
        send_gate[d] = wide[d * seqs : (d + 1) * seqs, :inner].astype(BF16)
    sixth = exchange(lambda other: send_gate.at[other], lambda j: recv_gate.at[j], s6, r6)

    wait(6, 7, 8, 9, 10, 11, 12, 13, 14, 16, 18, 21, 15)
    head_of = lax.broadcasted_iota(jnp.int32, (HEADS, inner), 1) // HEAD_DIM
    spreader = (head_of == lax.broadcasted_iota(jnp.int32, (HEADS, inner), 0)).astype(F32)

    total = send1[me].astype(F32)
    for j in range(1, n):
        first[j - 1].wait_recv()
        total = total + recv1[j].astype(F32)
    total = total.astype(BF16).astype(F32)

    def conv(now, past, taps):
        t = taps[...].astype(F32)
        p = past[...].astype(F32)
        acc = now * t[3:4]
        for k in range(3):
            acc = acc + p[k] * t[k : k + 1]
        return silu(acc)

    groups = GROUPS * STATE_DIM
    values = conv(total[:, offsets[1] - inner : offsets[1] - inner + inner], past_values, value_taps)
    writes = conv(total[:, offsets[2] - inner : offsets[2] - inner + groups], past_writes, write_taps)
    reads = conv(total[:, offsets[3] - inner : offsets[3] - inner + groups], past_reads, read_taps)
    raw = total[:, offsets[4] - inner : offsets[4] - inner + HEADS] + step_bias[...]
    step_size = jnp.maximum(raw, 0.0) + jnp.log1p(jnp.exp(-jnp.abs(raw)))
    decays = jnp.exp(-step_size * jnp.exp(decay_log[...]))
    pad = spread.shape[0] // 3
    spread[...] = jnp.zeros(spread.shape, F32)
    spread[0:seqs, :] = step_size
    spread[pad : pad + seqs, :] = decays
    spread[2 * pad : 2 * pad + 1, :] = skip_scale[...]
    per_channel = jnp.dot(
        spread[...], spreader, preferred_element_type=F32, precision=lax.Precision.HIGHEST
    )
    step_c = per_channel[0:seqs]
    decay_c = per_channel[pad : pad + seqs]
    skip_c = per_channel[2 * pad : 2 * pad + 1]
    half = inner // GROUPS
    for g in range(GROUPS):
        reads_g = reads[:, g * STATE_DIM : (g + 1) * STATE_DIM].astype(BF16)
        for s in range(seqs):
            block = state[s, g * half : (g + 1) * half, :].astype(BF16)
            seen = lax.dot_general(
                reads_g, block, (((1,), (1,)), ((), ())), preferred_element_type=F32
            )
            read_out[s : s + 1, g * half : (g + 1) * half] = seen[s : s + 1]
    drive = step_c * values
    decay_out[...] = jnp.zeros(decay_out.shape, F32)
    drive_out[...] = jnp.zeros(drive_out.shape, F32)
    write_out[...] = jnp.zeros(write_out.shape, F32)
    decay_out[0:seqs, :] = decay_c
    drive_out[0:seqs, :] = drive
    write_out[0:seqs, :] = writes
    base = decay_c * read_out[...] + skip_c * values
    gate = send_gate[me].astype(F32)
    for j in range(1, n):
        sixth[j - 1].wait_recv()
        gate = gate + recv_gate[j].astype(F32)
    gate_act = silu(gate.astype(BF16).astype(F32))
    product = writes * reads
    for g in range(GROUPS):
        here = slice(g * half, (g + 1) * half)
        overlap = jnp.sum(product[:, g * STATE_DIM : (g + 1) * STATE_DIM], -1, keepdims=True)
        gated = (base[:, here] + drive[:, here] * overlap) * gate_act[:, here]
        scale = lax.rsqrt(jnp.mean(gated * gated, -1, keepdims=True) + MIXER_EPSILON)
        mix_all[me, :, here] = (gated * scale * mixer_gain[:, here]).astype(BF16)
    second = exchange(lambda other: mix_all.at[me], lambda j: mix_all.at[me], s2, r2)

    strip = 256
    stores = []

    def update_states(g):
        @pl.loop(0, half // strip)
        def _(b):
            here = pl.ds(pl.multiple_of(g * half + b * strip, strip), strip)
            decay_t = jnp.transpose(decay_out[:, here])
            drive_t = jnp.transpose(drive_out[:, here])
            for s in range(seqs):
                write = write_out[s : s + 1, g * STATE_DIM : (g + 1) * STATE_DIM]
                state[s, here, :] = (
                    decay_t[:, s : s + 1] * state[s, here, :] + drive_t[:, s : s + 1] * write
                )

        where = pl.ds(g * half, half)
        store = pltpu.make_async_copy(
            state.at[:, where], state_out.at[:, where], store_sem.at[g]
        )
        store.start()
        stores.append(store)

    update_states(0)

    wait(17)
    for copy in second:
        copy.wait_recv()
    for d in range(n):
        mix_rows[d * seqs : (d + 1) * seqs, :] = mix_all[d].astype(F32)
    mix_out = jnp.dot(mix_rows[...].astype(BF16), out_w[...], preferred_element_type=F32)
    residual = RESIDUAL_SCALE * x[...].astype(F32) + mix_out.astype(BF16).astype(F32)
    res_all[me] = residual.astype(BF16)
    kv, tp = lax.axis_index("kv"), lax.axis_index("tp")
    chips = n // tp_size

    def to_device(block, send_sem, recv_sem, chip, core):
        copy = pltpu.make_async_remote_copy(
            src_ref=res_all.at[block],
            dst_ref=res_all.at[block],
            send_sem=send_sem,
            recv_sem=recv_sem,
            device_id={"kv": chip, "tp": core},
            device_id_type=pl.DeviceIdType.MESH,
        )
        copy.start()
        return copy

    far = [
        to_device(me, s3.at[j], r3.at[j], lax.rem(kv + j, chips), tp) for j in range(1, chips)
    ]
    near = [
        to_device(me, s7.at[0, c], r7.at[0, c], kv, lax.rem(tp + c, tp_size))
        for c in range(1, tp_size)
    ]
    for g in range(1, GROUPS):
        update_states(g)

    for j in range(1, chips):
        far[j - 1].wait_recv()
        block = lax.rem(kv + chips - j, chips) * tp_size + tp
        near += [
            to_device(block, s7.at[j, c], r7.at[j, c], kv, lax.rem(tp + c, tp_size))
            for c in range(1, tp_size)
        ]
    for copy in near:
        copy.wait_recv()
    total1 = jnp.zeros((rows, 1), F32)
    for d in range(n):
        total1 = total1 + jnp.sum(res_all[d].astype(F32), -1, keepdims=True)
    average = total1 / model
    total2 = jnp.zeros((rows, 1), F32)
    for d in range(n):
        off = res_all[d].astype(F32) - average
        total2 = total2 + jnp.sum(off * off, -1, keepdims=True)
    scale = lax.rsqrt(total2 / model + NORM_EPSILON)
    for d in range(n):
        here = slice(d * cols, (d + 1) * cols)
        block = (res_all[d].astype(F32) - average) * scale * gain1[:, here]
        normed_b[:, here] = block.astype(BF16)
        normed_f[:, here] = block.astype(BF16).astype(F32)
    for d in range(n):

        @pl.when(me == d)
        def _():
            own_normed[...] = normed_f[d * seqs : (d + 1) * seqs, :]

    wait(19, 20)
    chunk = min(512, up_w.shape[1])

    @pl.loop(0, up_w.shape[1] // chunk)
    def _(c):
        here = pl.ds(pl.multiple_of(c * chunk, chunk), chunk)
        h = jnp.dot(normed_b[...], up_w[:, here], preferred_element_type=F32)
        h = jnp.maximum(h, 0.0)
        hidden[:, here] = (h * h).astype(BF16)

    span = model // halves
    fourth = []
    for part in range(halves):

        @pl.loop(0, span // 512)
        def _(c):
            there = pl.ds(pl.multiple_of(c * 512, 512), 512)
            here = pl.ds(pl.multiple_of(part * span + c * 512, 512), 512)
            down_rows[:, there] = jnp.dot(
                hidden[...], down_w[:, here], preferred_element_type=F32
            )

        for d in range(n):
            send2[part, d] = down_rows[d * seqs : (d + 1) * seqs, :].astype(BF16)
        fourth.append(
            exchange(
                lambda other: send2.at[part, other],
                lambda j: recv2.at[part, j],
                s4.at[part],
                r4.at[part],
            )
        )

    rows2 = []
    for part in range(halves):
        channel = send2[part, me].astype(F32)
        for j in range(1, n):
            fourth[part][j - 1].wait_recv()
            channel = channel + recv2[part, j].astype(F32)
        rows2.append(
            RESIDUAL_SCALE * own_normed[:, part * span : (part + 1) * span]
            + channel.astype(BF16).astype(F32)
        )
    average = sum(jnp.sum(r, -1, keepdims=True) for r in rows2) / model
    rows2 = [r - average for r in rows2]
    variance = sum(jnp.sum(r * r, -1, keepdims=True) for r in rows2) / model
    scale = lax.rsqrt(variance + NORM_EPSILON)
    for d in range(n):
        part, begin = divmod(d * cols, span)
        block = rows2[part][:, begin : begin + cols] * scale * gain2[:, d * cols : (d + 1) * cols]
        finished[d] = block.astype(BF16)
    done_all[me] = finished[me]
    fifth = exchange(lambda other: finished.at[other], lambda j: done_all.at[me], s5, r5)
    for copy in fifth:
        copy.wait_recv()
    for d in range(n):
        done_rows[d * seqs : (d + 1) * seqs, :] = done_all[d].astype(F32)
    layer_out[...] = done_rows[...].astype(BF16)
    for store in stores:
        store.wait()
    for group in [first, sixth, second, far, near, *fourth, fifth]:
        for copy in group:
            copy.wait_send()


def tail_kernel(rows_in, state_in, rows_out, state_out, rows_held, state_held, in_sem, out_sem):
    seqs, depth = state_in.shape[0], state_in.shape[1] // 2
    pieces = []
    for s in range(seqs):
        for part in range(2):
            here = (s, pl.ds(part * depth, depth))
            pieces.append((state_in.at[here], state_held.at[here], state_out.at[here]))
    pieces.append((rows_in, rows_held, rows_out))
    loads = [
        pltpu.make_async_copy(src, mid, in_sem.at[i]) for i, (src, mid, _) in enumerate(pieces)
    ]
    stores = [
        pltpu.make_async_copy(mid, dst, out_sem.at[i]) for i, (_, mid, dst) in enumerate(pieces)
    ]
    for copy in loads:
        copy.start()
    for load, store in zip(loads, stores):
        load.wait()
        store.start()
    for copy in stores:
        copy.wait()


def on_device(n, tp_size, *args):
    x = args[0]
    state = args[15]
    seqs, rows, cols = state.shape[0], x.shape[0], x.shape[1]
    inner = args[1].shape[1]
    model = args[18].shape[0]
    hidden_here = args[19].shape[1]
    offsets = [0]
    for i in range(1, 5):
        offsets.append(offsets[-1] + args[i].shape[1])
    width = offsets[-1] + 128
    args = list(args)
    args[15] = state.reshape(seqs, inner, STATE_DIM)
    args[5] = args[5].T
    for i in (9, 10, 11):
        args[i] = jnp.transpose(args[i], (1, 0, 2))
    for i in (12, 13, 14, 16, 18, 21):
        args[i] = args[i].reshape(1, -1)
    ways, halves = 4, 4
    chips = n // tp_size
    pad = (seqs + 7) // 8 * 8
    dma = pltpu.SemaphoreType.DMA
    scratch = [pltpu.VMEM(a.shape, a.dtype) for a in args]
    scratch += [
        pltpu.VMEM((pad, inner), F32),
        pltpu.VMEM((pad, inner), F32),
        pltpu.VMEM((pad, GROUPS * STATE_DIM), F32),
        pltpu.VMEM((rows, width), F32),
        pltpu.VMEM((n, seqs, width - inner), BF16),
        pltpu.VMEM((n, seqs, width - inner), BF16),
        pltpu.VMEM((n, seqs, inner), BF16),
        pltpu.VMEM((n, seqs, inner), BF16),
        pltpu.VMEM((3 * pad, HEADS), F32),
        pltpu.VMEM((seqs, inner), F32),
        pltpu.VMEM((n, seqs, inner), BF16),
        pltpu.VMEM((rows, inner), F32),
        pltpu.VMEM((n, rows, cols), BF16),
        pltpu.VMEM((rows, model), F32),
        pltpu.VMEM((seqs, model), F32),
        pltpu.VMEM((rows, model), BF16),
        pltpu.VMEM((rows, hidden_here), BF16),
        pltpu.VMEM((rows, model // halves), F32),
        pltpu.VMEM((halves, n, seqs, model // halves), BF16),
        pltpu.VMEM((halves, n, seqs, model // halves), BF16),
        pltpu.VMEM((n, seqs, cols), BF16),
        pltpu.VMEM((n, seqs, cols), BF16),
        pltpu.VMEM((rows, cols), F32),
        dma((20 + 2 * ways,)),
        dma((GROUPS,)),
        dma((n,)), dma((n,)), dma((n,)), dma((n,)), dma((n,)), dma((n,)),
        dma((halves, n)), dma((halves, n)), dma((n,)), dma((n,)), dma((n,)), dma((n,)),
        dma((chips, tp_size)), dma((chips, tp_size)),
    ]
    geo = (n, tp_size, seqs, rows, width, tuple(offsets), ways, halves)
    result, state_next = pl.pallas_call(
        functools.partial(layer_kernel, geo),
        out_shape=(
            jax.ShapeDtypeStruct((rows, cols), BF16),
            jax.ShapeDtypeStruct((seqs, inner, STATE_DIM), F32),
        ),
        in_specs=[ANY] * 22,
        out_specs=(VMEM, ANY),
        scratch_shapes=scratch,
        compiler_params=pltpu.CompilerParams(
            collective_id=0, has_side_effects=True, vmem_limit_bytes=67043328
        ),
        name="layer",
    )(*args)
    result, state_next = pl.pallas_call(
        tail_kernel,
        out_shape=(
            jax.ShapeDtypeStruct(result.shape, BF16),
            jax.ShapeDtypeStruct(state_next.shape, F32),
        ),
        in_specs=[ANY] * 2,
        out_specs=(ANY, ANY),
        scratch_shapes=[
            pltpu.VMEM(result.shape, BF16),
            pltpu.VMEM(state_next.shape, F32),
            dma((2 * seqs + 1,)),
            dma((2 * seqs + 1,)),
        ],
        compiler_params=pltpu.CompilerParams(vmem_limit_bytes=67043328),
        name="tail",
    )(result, state_next)
    return result, state_next.reshape(state.shape)


def solution(mesh):
    tp_size = mesh.shape["tp"]
    n = mesh.shape["kv"] * tp_size
    split, whole = P(("kv", "tp"), None), P()
    past = P(("dp", "kv", "tp"), None, None)
    states = P(("dp", "kv", "tp"), None, None, None)
    columns = P(None, ("kv", "tp"))
    placed = (
        (P("dp", ("kv", "tp")),) + (split,) * 5 + (whole,) * 3 + (past,) * 3 + (whole,) * 3
        + (states, whole, columns, whole, columns, split, whole)
    )
    return jax.shard_map(
        functools.partial(on_device, n, tp_size),
        mesh=mesh,
        in_specs=placed,
        out_specs=(P("dp", ("kv", "tp")), states),
        check_vma=False,
    )
```
